32 devices in a mesh: grp: 2 (over x), kv: 4 (over z), tp: 4 (over y, core).
Axes of the slice: x: 2, y: 2, z: 4, core: 2. Of those that a mesh axis runs over, the one named last changes fastest.
Arguments:
- stream: bfloat16 [32, 4096], P('grp', ('kv', 'tp')), parts along dimension 0, may hold values from -6 to 6
- attn_gain: bfloat16 [4096], P('kv'), may hold values from 0.099609375 to 1.8984375
- mlp_gain: bfloat16 [4096], P('kv'), may hold values from 0.099609375 to 1.8984375
- w_query: bfloat16 [4096, 4096], P('kv', 'tp'), may hold values from -0.09375 to 0.09375
- w_key: bfloat16 [4096, 4096], P('kv', 'tp'), may hold values from -0.09375 to 0.09375
- w_value: bfloat16 [4096, 4096], P('kv', 'tp'), may hold values from -0.09375 to 0.09375
- w_zgate: bfloat16 [4096, 4096], P('kv', 'tp'), may hold values from -0.09375 to 0.09375
- w_decay: bfloat16 [4096, 32], P('kv'), may hold values from -0.09375 to 0.09375
- w_beta: bfloat16 [4096, 32], P('kv'), may hold values from -0.09375 to 0.09375
- decay_rate: float32 [32], P('tp'), may hold values from 0.03 to 3
- head_gain: float32 [128], replicated, may hold values from 0.1 to 1.9
- w_attn_out: bfloat16 [4096, 4096], P('tp', 'kv'), may hold values from -0.09375 to 0.09375
- w_gate: bfloat16 [4096, 11264], P('kv', 'tp'), may hold values from -0.09375 to 0.09375
- w_up: bfloat16 [4096, 11264], P('kv', 'tp'), may hold values from -0.09375 to 0.09375
- w_down: bfloat16 [11264, 4096], P('tp', 'kv'), may hold values from -0.0546875 to 0.0546875
- state: float32 [32, 32, 128, 128], P(('grp', 'kv'), 'tp'), parts along dimension 0, may hold values from -4 to 4
Outputs:
- next_stream: bfloat16 [32, 4096], P('grp', ('kv', 'tp')), parts along dimension 0
- new_state: float32 [32, 32, 128, 128], P(('grp', 'kv'), 'tp'), parts along dimension 0
The draws below stay inside these ranges and needn't reach their ends.
There are 2 independent parts, one for each index of `grp`. The reference program is written for one: setup_inputs(seed, part) draws one part's arguments, and reference() takes and returns one part's arrays. A program takes and returns all parts, laid end to end along the dimension named above; an argument that names none is the same for every part. Nothing has to cross between parts.
All inputs are finite; a program needn't handle non-finite values.
Results may differ from the reference program's by a relative error of at most 0.025.
Values may be sent and summed in bfloat16 or wider, within the bound.
No kernel may reach another device: no remote copies, remote signals or barrier semaphores. Data moves between devices by JAX's collectives and lax.ppermute only.
A program may use at most 64 MiB of HBM per device.

```python
import math
import jax
import jax.numpy as jnp
from jax import lax

D = 4096
HEADS = 32
HEAD_DIM = 128
FF = 11264
BATCH = 16


def block_scale(rng, dims, pieces, least, top_value):
    level = 1.0
    for axis_at, parts in pieces:
        steps = jax.random.uniform(jax.random.fold_in(jax.random.fold_in(rng, 6), axis_at), (parts,), jnp.float32, least / len(pieces), top_value / len(pieces))
        level = level * jnp.repeat(jnp.exp(steps), dims[axis_at] // parts).reshape((-1,) + (1,) * (len(dims) - 1 - axis_at))
    return level


def centred(rng, extent, width, bound, split=(), dtype=jnp.bfloat16):
    result = width * jax.random.normal(rng, extent, jnp.float32)
    if split:
        result = result * block_scale(rng, extent, split, -0.22, 0.18)
    return jnp.clip(result, -bound, bound).astype(dtype)


def setup_inputs(seed: int = 0, part: int = 0) -> dict:
    seeds = jax.random.split(jax.random.key(seed), 17)
    own_keys = jax.random.split(jax.random.fold_in(seeds[16], part), 17)
    return {
        "stream": centred(own_keys[0], (BATCH, D), 1.0, 6.0, ((1, 16),)),
        "attn_gain": jnp.clip(1.0 + 0.18 * jax.random.normal(seeds[1], (D,), jnp.float32), 0.099609375, 1.8984375).astype(jnp.bfloat16),
        "mlp_gain": jnp.clip(1.0 + 0.18 * jax.random.normal(seeds[2], (D,), jnp.float32), 0.099609375, 1.8984375).astype(jnp.bfloat16),
        "w_query": centred(seeds[3], (D, HEADS * HEAD_DIM), D ** -0.5, 0.09375, ((0, 4), (1, 4))),
        "w_key": centred(seeds[4], (D, HEADS * HEAD_DIM), D ** -0.5, 0.09375, ((0, 4), (1, 4))),
        "w_value": centred(seeds[5], (D, HEADS * HEAD_DIM), D ** -0.5, 0.09375, ((0, 4), (1, 4))),
        "w_zgate": centred(seeds[6], (D, HEADS * HEAD_DIM), D ** -0.5, 0.09375, ((0, 4), (1, 4))),
        "w_decay": centred(seeds[7], (D, HEADS), D ** -0.5, 0.09375, ((0, 4),)),
        "w_beta": centred(seeds[8], (D, HEADS), D ** -0.5, 0.09375, ((0, 4),)),
        "decay_rate": jnp.clip(jnp.exp(math.log(3.0) - 4.6051702 * jax.random.uniform(seeds[9], (HEADS,), jnp.float32) ** block_scale(seeds[9], (HEADS,), ((0, 4),), -0.2, 0.2)), 0.03, 3.0),
        "head_gain": jnp.clip(1.0 + 0.18 * jax.random.normal(seeds[10], (HEAD_DIM,), jnp.float32), 0.1, 1.9),
        "w_attn_out": centred(seeds[11], (HEADS * HEAD_DIM, D), (HEADS * HEAD_DIM) ** -0.5, 0.09375, ((0, 4), (1, 4))),
        "w_gate": centred(seeds[12], (D, FF), D ** -0.5, 0.09375, ((0, 4), (1, 4))),
        "w_up": centred(seeds[13], (D, FF), D ** -0.5, 0.09375, ((0, 4), (1, 4))),
        "w_down": centred(seeds[14], (FF, D), FF ** -0.5, 0.0546875, ((0, 4), (1, 4))),
        "state": centred(own_keys[15], (BATCH, HEADS, HEAD_DIM, HEAD_DIM), 0.3, 4.0, ((0, 4), (1, 4)), jnp.float32),
    }


EPSILON = 1e-06

def l2_unit(values):
    return values * lax.rsqrt(lax.optimization_barrier(jnp.sum(values * values, axis=-1, keepdims=True)) + EPSILON)

def delta_update(query, key_vec, value_vec, log_decay, beta_gate, state):
    decayed = jnp.exp(log_decay)[..., None, None] * state
    recalled = jnp.einsum('shkv,shk->shv', decayed, key_vec, precision=lax.Precision.HIGHEST)
    update = beta_gate[..., None] * (value_vec - recalled)
    new_state = decayed + key_vec[..., :, None] * update[..., None, :]
    head_out = jnp.einsum('shkv,shk->shv', new_state, query, precision=lax.Precision.HIGHEST)
    return (new_state, head_out)

def head_mix(head_out, head_gain, z_gate):
    scaled = head_out * lax.rsqrt(lax.optimization_barrier(jnp.mean(head_out * head_out, axis=-1, keepdims=True)) + EPSILON)
    return (scaled * head_gain.astype(jnp.float32) * jax.nn.silu(z_gate)).astype(jnp.bfloat16)

def reference(stream, attn_gain, mlp_gain, w_query, w_key, w_value, w_zgate, w_decay, w_beta, decay_rate, head_gain, w_attn_out, w_gate, w_up, w_down, state):
    batch = stream.shape[0]
    stream_f = stream.astype(jnp.float32)
    row_scale = lax.rsqrt(lax.optimization_barrier(jnp.mean(stream_f * stream_f, axis=1, keepdims=True)) + EPSILON)
    normed = (stream_f * attn_gain.astype(jnp.float32)[None, :]).astype(jnp.bfloat16)

    def project(weight):
        return jnp.dot(normed, weight, preferred_element_type=jnp.float32) * row_scale
    query = l2_unit(project(w_query).reshape(batch, HEADS, HEAD_DIM)) * HEAD_DIM ** (-0.5)
    key_vec = l2_unit(project(w_key).reshape(batch, HEADS, HEAD_DIM))
    value_vec = project(w_value).reshape(batch, HEADS, HEAD_DIM)
    z_gate = project(w_zgate).reshape(batch, HEADS, HEAD_DIM)
    log_decay = -decay_rate[None, :] * jax.nn.softplus(project(w_decay))
    beta_gate = jax.nn.sigmoid(project(w_beta))
    new_state, head_out = delta_update(query, key_vec, value_vec, log_decay, beta_gate, state)
    mixed = head_mix(head_out, head_gain, z_gate).reshape(batch, HEADS * HEAD_DIM)
    residual_stream = (stream_f + jnp.dot(mixed, w_attn_out, preferred_element_type=jnp.float32)).astype(jnp.bfloat16)
    resid_f = residual_stream.astype(jnp.float32)
    mlp_scale = lax.rsqrt(lax.optimization_barrier(jnp.mean(resid_f * resid_f, axis=1, keepdims=True)) + EPSILON)
    normed_mlp = (resid_f * mlp_gain.astype(jnp.float32)[None, :]).astype(jnp.bfloat16)
    gate = jnp.dot(normed_mlp, w_gate, preferred_element_type=jnp.float32) * mlp_scale
    up_proj = jnp.dot(normed_mlp, w_up, preferred_element_type=jnp.float32) * mlp_scale
    hidden = (jax.nn.silu(gate) * up_proj).astype(jnp.bfloat16)
    next_stream = (resid_f + jnp.dot(hidden, w_down, preferred_element_type=jnp.float32)).astype(jnp.bfloat16)
    return (next_stream, new_state)
```

```python
import jax
import jax.numpy as jnp
from jax import lax
from jax.sharding import PartitionSpec as P


D = 4096
HEAD_DIM = 128


EPSILON = 1e-06


def l2_unit(values):
    return values * lax.rsqrt(jnp.sum(values * values, axis=-1, keepdims=True) + EPSILON)


def delta_update(query, key_vec, value_vec, log_decay, beta_gate, state):
    decayed = jnp.exp(log_decay)[..., None, None] * state
    recalled = jnp.einsum("shkv,shk->shv", decayed, key_vec, precision=lax.Precision.HIGHEST)
    update = beta_gate[..., None] * (value_vec - recalled)
    new_state = decayed + key_vec[..., :, None] * update[..., None, :]
    head_out = jnp.einsum("shkv,shk->shv", new_state, query, precision=lax.Precision.HIGHEST)
    return (new_state, head_out)


def head_mix(head_out, head_gain, z_gate):
    scaled = head_out * lax.rsqrt(jnp.mean(head_out * head_out, axis=-1, keepdims=True) + EPSILON)
    return (scaled * head_gain * jax.nn.silu(z_gate)).astype(jnp.bfloat16)


def peers(axis):
    return lax.axis_index(axis), lax.axis_size(axis)


def spread(values, axis):
    me, size = peers(axis)
    moved = [
        lax.ppermute(values, axis, [(i, (i + shift) % size) for i in range(size)])
        for shift in range(1, size)
    ]
    return [values] + moved


def gather(values, axis, dim):
    me, size = peers(axis)
    found = spread(values, axis)
    width = values.shape[dim]
    shape = list(values.shape)
    shape[dim] = width * size
    out = jnp.zeros(shape, values.dtype)
    for shift, piece in enumerate(found):
        out = lax.dynamic_update_slice_in_dim(out, piece, (me - shift) % size * width, dim)
    return out


def scatter_sum(values, axis, dim):
    me, size = peers(axis)
    width = values.shape[dim] // size
    total = None
    for shift in range(size):
        piece = lax.dynamic_slice_in_dim(values, (me + shift) % size * width, width, dim)
        if shift:
            piece = lax.ppermute(piece, axis, [(i, (i + shift) % size) for i in range(size)])
        piece = piece.astype(jnp.float32)
        total = piece if total is None else total + piece
    return total


def halves(values):
    high = values.astype(jnp.bfloat16)
    low = (values - lax.reduce_precision(values, 8, 7)).astype(jnp.bfloat16)
    return jnp.stack([high, low], axis=1)


def local(
    stream,
    attn_gain,
    mlp_gain,
    w_query,
    w_key,
    w_value,
    w_zgate,
    w_decay,
    w_beta,
    decay_rate,
    head_gain,
    w_attn_out,
    w_gate,
    w_up,
    w_down,
    state,
):
    seq_count = state.shape[0]
    local_heads = state.shape[1]
    width = w_query.shape[1]
    hidden_width = w_gate.shape[1]
    head_offset = lax.axis_index("tp") * local_heads
    block_rows = gather(stream, "tp", 1).astype(jnp.float32)
    local_squares = jnp.sum(block_rows * block_rows, axis=1)
    normed = (block_rows * attn_gain.astype(jnp.float32)[None, :]).astype(jnp.bfloat16)
    pieces = [
        jnp.dot(normed, weight, preferred_element_type=jnp.float32)
        for weight in (w_query, w_key, w_value, w_zgate)
    ]
    pieces += [
        lax.dynamic_slice_in_dim(
            jnp.dot(normed, weight, preferred_element_type=jnp.float32),
            head_offset,
            local_heads,
            1,
        )
        for weight in (w_decay, w_beta)
    ]
    summed = scatter_sum(
        jnp.concatenate(
            [piece.astype(jnp.bfloat16) for piece in pieces] + [halves(local_squares)], axis=1
        ),
        "kv",
        0,
    )
    row_scale = lax.rsqrt(jnp.sum(summed[:, -2:], axis=1, keepdims=True) / D + EPSILON)
    summed = summed * row_scale

    def head_block(index):
        return summed[:, index * width : (index + 1) * width].reshape(
            seq_count, local_heads, HEAD_DIM
        )

    query = l2_unit(head_block(0)) * HEAD_DIM ** (-0.5)
    key_vec = l2_unit(head_block(1))
    value_vec = head_block(2)
    z_gate = head_block(3)
    log_decay = -decay_rate[None, :] * jax.nn.softplus(
        summed[:, 4 * width : 4 * width + local_heads]
    )
    beta_gate = jax.nn.sigmoid(summed[:, 4 * width + local_heads : 4 * width + 2 * local_heads])
    new_state, head_out = delta_update(query, key_vec, value_vec, log_decay, beta_gate, state)
    mixed = head_mix(head_out, head_gain, z_gate).reshape(seq_count, width)
    attn_part = jnp.dot(
        gather(mixed, "kv", 0),
        w_attn_out,
        preferred_element_type=jnp.float32,
    )
    attn_sum = sum(
        part.astype(jnp.float32) for part in spread(attn_part.astype(jnp.bfloat16), "tp")
    )
    mlp_block = (block_rows + attn_sum).astype(jnp.bfloat16).astype(jnp.float32)
    mlp_local_squares = jnp.sum(mlp_block * mlp_block, axis=1)
    normed_mlp = (mlp_block * mlp_gain.astype(jnp.float32)[None, :]).astype(jnp.bfloat16)
    gate_part = jnp.dot(normed_mlp, w_gate, preferred_element_type=jnp.float32)
    up_part = jnp.dot(normed_mlp, w_up, preferred_element_type=jnp.float32)
    totals = scatter_sum(
        jnp.concatenate(
            [
                gate_part.astype(jnp.bfloat16),
                up_part.astype(jnp.bfloat16),
                halves(mlp_local_squares),
            ],
            axis=1,
        ),
        "kv",
        0,
    )
    mlp_scale = lax.rsqrt(jnp.sum(totals[:, -2:], axis=1, keepdims=True) / D + EPSILON)
    gate_sum = totals[:, :hidden_width] * mlp_scale
    up_sum = totals[:, hidden_width : 2 * hidden_width] * mlp_scale
    hidden = gather((jax.nn.silu(gate_sum) * up_sum).astype(jnp.bfloat16), "kv", 0)
    down_part = jnp.dot(hidden, w_down, preferred_element_type=jnp.float32)
    mlp_sum = scatter_sum(down_part.astype(jnp.bfloat16), "tp", 1)
    out_width = stream.shape[1]
    residual_own = lax.dynamic_slice_in_dim(
        mlp_block, lax.axis_index("tp") * out_width, out_width, 1
    )
    next_stream = (residual_own + mlp_sum).astype(jnp.bfloat16)
    return (next_stream, new_state)


def solution(mesh):
    return jax.shard_map(
        local,
        mesh=mesh,
        in_specs=(
            P("grp", ("kv", "tp")),
            P("kv"),
            P("kv"),
            P("kv", "tp"),
            P("kv", "tp"),
            P("kv", "tp"),
            P("kv", "tp"),
            P("kv", None),
            P("kv", None),
            P("tp"),
            P(),
            P("tp", "kv"),
            P("kv", "tp"),
            P("kv", "tp"),
            P("tp", "kv"),
            P(("grp", "kv"), "tp", None, None),
        ),
        out_specs=(P("grp", ("kv", "tp")), P(("grp", "kv"), "tp", None, None)),
        check_vma=False,
    )
```

```python
import jax
import jax.numpy as jnp
from jax import lax
from jax.sharding import PartitionSpec as P


D = 4096
HEAD_DIM = 128


EPSILON = 1e-06


def l2_unit(values):
    return values * lax.rsqrt(jnp.sum(values * values, axis=-1, keepdims=True) + EPSILON)


def delta_update(query, key_vec, value_vec, log_decay, beta_gate, state):
    decay = jnp.exp(log_decay)[..., None]
    recalled = decay * jnp.sum(state * key_vec[..., :, None], axis=2)
    read = decay * jnp.sum(state * query[..., :, None], axis=2)
    update = beta_gate[..., None] * (value_vec - recalled)
    new_state = decay[..., None] * state + key_vec[..., :, None] * update[..., None, :]
    head_out = read + jnp.sum(key_vec * query, axis=-1, keepdims=True) * update
    return (new_state, head_out)


def head_mix(head_out, head_gain, z_gate):
    scaled = head_out * lax.rsqrt(jnp.mean(head_out * head_out, axis=-1, keepdims=True) + EPSILON)
    return (scaled * head_gain * jax.nn.silu(z_gate)).astype(jnp.bfloat16)


def partners(axis):
    size = lax.axis_size(axis)
    if size & (size - 1):
        return [[(i, (i + shift) % size) for i in range(size)] for shift in range(1, size)]
    return [[(i, i ^ shift) for i in range(size)] for shift in reversed(range(1, size))]


def offset(axis, index, back=False):
    me, size = lax.axis_index(axis), lax.axis_size(axis)
    if size & (size - 1):
        return (me - 1 - index) % size if back else (me + 1 + index) % size
    return me ^ (size - 1 - index)


def spread(values, axis):
    return [values] + [lax.ppermute(values, axis, pairs) for pairs in partners(axis)]


def gather(values, axis, dim):
    me, size = lax.axis_index(axis), lax.axis_size(axis)
    found = spread(values, axis)
    width = values.shape[dim]
    shape = list(values.shape)
    shape[dim] = width * size
    out = jnp.zeros(shape, values.dtype)
    out = lax.dynamic_update_slice_in_dim(out, values, me * width, dim)
    for index, piece in enumerate(found[1:]):
        out = lax.dynamic_update_slice_in_dim(out, piece, offset(axis, index, True) * width, dim)
    return out


def scatter_sum(values, axis, dim):
    me, size = lax.axis_index(axis), lax.axis_size(axis)
    width = values.shape[dim] // size
    total = None
    for index, pairs in enumerate(partners(axis)):
        piece = lax.dynamic_slice_in_dim(values, offset(axis, index) * width, width, dim)
        piece = lax.ppermute(piece, axis, pairs).astype(jnp.float32)
        total = piece if total is None else total + piece
    own = lax.dynamic_slice_in_dim(values, me * width, width, dim).astype(jnp.float32)
    return own if total is None else total + own


def near_copy(weight):
    one = lax.optimization_barrier(jnp.ones((), weight.dtype))
    return lax.optimization_barrier(weight * one)


def halves(values):
    high = values.astype(jnp.bfloat16)
    low = (values - lax.reduce_precision(values, 8, 7)).astype(jnp.bfloat16)
    return jnp.stack([high, low], axis=1)


def local(
    stream,
    attn_gain,
    mlp_gain,
    w_query,
    w_key,
    w_value,
    w_zgate,
    w_decay,
    w_beta,
    decay_rate,
    head_gain,
    w_attn_out,
    w_gate,
    w_up,
    w_down,
    state,
):
    seq_count = state.shape[0]
    local_heads = state.shape[1]
    width = w_query.shape[1]
    hidden_width = w_gate.shape[1]
    head_offset = lax.axis_index("tp") * local_heads
    small_weights = lax.optimization_barrier(jnp.concatenate([w_decay, w_beta], axis=1))
    block_rows = gather(stream, "tp", 1).astype(jnp.float32)
    local_squares = jnp.sum(block_rows * block_rows, axis=1)
    normed = (block_rows * attn_gain.astype(jnp.float32)[None, :]).astype(jnp.bfloat16)
    pieces = [
        jnp.dot(normed, weight, preferred_element_type=jnp.float32)
        for weight in (w_query, w_key, w_value, w_zgate)
    ]
    small = jnp.dot(normed, small_weights, preferred_element_type=jnp.float32)
    pieces += [
        lax.dynamic_slice_in_dim(small, start + head_offset, local_heads, 1)
        for start in (0, w_decay.shape[1])
    ]
    summed = scatter_sum(
        jnp.concatenate(
            [piece.astype(jnp.bfloat16) for piece in pieces] + [halves(local_squares)], axis=1
        ),
        "kv",
        0,
    )
    row_scale = lax.rsqrt(jnp.sum(summed[:, -2:], axis=1, keepdims=True) / D + EPSILON)
    summed = summed * row_scale

    def head_block(index):
        return summed[:, index * width : (index + 1) * width].reshape(
            seq_count, local_heads, HEAD_DIM
        )

    query = l2_unit(head_block(0)) * HEAD_DIM ** (-0.5)
    key_vec = l2_unit(head_block(1))
    value_vec = head_block(2)
    z_gate = head_block(3)
    log_decay = -decay_rate[None, :] * jax.nn.softplus(
        summed[:, 4 * width : 4 * width + local_heads]
    )
    beta_gate = jax.nn.sigmoid(summed[:, 4 * width + local_heads : 4 * width + 2 * local_heads])
    new_state, head_out = delta_update(query, key_vec, value_vec, log_decay, beta_gate, state)
    mixed = head_mix(head_out, head_gain, z_gate).reshape(seq_count, width)
    attn_part = jnp.dot(
        gather(mixed, "kv", 0),
        w_attn_out,
        preferred_element_type=jnp.float32,
    )
    attn_sum = sum(
        part.astype(jnp.float32) for part in spread(attn_part.astype(jnp.bfloat16), "tp")
    )
    mlp_block = (block_rows + attn_sum).astype(jnp.bfloat16).astype(jnp.float32)
    mlp_local_squares = jnp.sum(mlp_block * mlp_block, axis=1)
    normed_mlp = (mlp_block * mlp_gain.astype(jnp.float32)[None, :]).astype(jnp.bfloat16)
    gate_part = jnp.dot(normed_mlp, near_copy(w_gate), preferred_element_type=jnp.float32)
    up_part = jnp.dot(normed_mlp, w_up, preferred_element_type=jnp.float32)
    totals = scatter_sum(
        jnp.concatenate(
            [
                gate_part.astype(jnp.bfloat16),
                up_part.astype(jnp.bfloat16),
                halves(mlp_local_squares),
            ],
            axis=1,
        ),
        "kv",
        0,
    )
    mlp_scale = lax.rsqrt(jnp.sum(totals[:, -2:], axis=1, keepdims=True) / D + EPSILON)
    gate_sum = totals[:, :hidden_width] * mlp_scale
    up_sum = totals[:, hidden_width : 2 * hidden_width] * mlp_scale
    hidden = gather((jax.nn.silu(gate_sum) * up_sum).astype(jnp.bfloat16), "kv", 0)
    down_part = jnp.dot(hidden, near_copy(w_down), preferred_element_type=jnp.float32)
    mlp_sum = scatter_sum(down_part.astype(jnp.bfloat16), "tp", 1)
    out_width = stream.shape[1]
    residual_own = lax.dynamic_slice_in_dim(
        mlp_block, lax.axis_index("tp") * out_width, out_width, 1
    )
    next_stream = (residual_own + mlp_sum).astype(jnp.bfloat16)
    return (next_stream, new_state)


def solution(mesh):
    return jax.shard_map(
        local,
        mesh=mesh,
        in_specs=(
            P("grp", ("kv", "tp")),
            P("kv"),
            P("kv"),
            P("kv", "tp"),
            P("kv", "tp"),
            P("kv", "tp"),
            P("kv", "tp"),
            P("kv", None),
            P("kv", None),
            P("tp"),
            P(),
            P("tp", "kv"),
            P("kv", "tp"),
            P("kv", "tp"),
            P("tp", "kv"),
            P(("grp", "kv"), "tp", None, None),
        ),
        out_specs=(P("grp", ("kv", "tp")), P(("grp", "kv"), "tp", None, None)),
        check_vma=False,
    )
```
